32 devices in a mesh: sp: 8 (over z, y), tp: 4 (over x, core).
Axes of the slice: x: 2, y: 2, z: 4, core: 2. Of those that a mesh axis runs over, the one named last changes fastest.
Arguments:
- memory_queries: bfloat16 [2048, 768], P('sp', 'tp'), may hold values from -6 to 6
- memory_keys: bfloat16 [2048, 768], P('sp', 'tp'), may hold values from -6 to 6
- memory_values: bfloat16 [2048, 768], P('sp', 'tp'), may hold values from -6 to 6
- output_gate_preactivation: bfloat16 [2048, 768], P('sp', 'tp'), may hold values from -6 to 6
- log_input_gate: float32 [8, 2048], P('tp', 'sp'), may hold values from -4 to 300
- forget_preactivation: float32 [8, 2048], P('tp', 'sp'), may hold values from -5 to 5
- head_forget_bias: float32 [8], P('tp'), may hold values from 3 to 16
- forget_extra_boost: float32 [8, 2048], P('tp', 'sp'), may hold values from -2 to 0
- head_norm_gain: float32 [768], P('tp'), may hold values from 0.1 to 1.9
- memory_output_weight: bfloat16 [768, 2048], replicated, may hold values from -0.21875 to 0.21875
- residual: bfloat16 [2048, 2048], P('sp'), may hold values from -6 to 6
- expert_norm_gain: float32 [2048], replicated, may hold values from 0.1 to 1.9
- routes: int32 [2048, 4], P('sp'), may hold values from 0 to 31, all different within a row; in each aligned block of 256 rows (0 to 255, 256 to 511, ...) at most 64 rows name the same one
- router_weight_matrix: float32 [2048, 4], P('sp'), may hold values from 0.1 to 1
- routed_gate_weight: bfloat16 [32, 2048, 512], P('sp', None, 'tp'), may hold values from -0.125 to 0.125
- routed_up_weight: bfloat16 [32, 2048, 512], P('sp', None, 'tp'), may hold values from -0.125 to 0.125
- routed_down_weight: bfloat16 [32, 512, 2048], P('sp', 'tp'), may hold values from -0.25 to 0.25
- shared_gate_weight: bfloat16 [2048, 512], P(None, 'tp'), may hold values from -0.125 to 0.125
- shared_up_weight: bfloat16 [2048, 512], P(None, 'tp'), may hold values from -0.125 to 0.125
- shared_down_weight: bfloat16 [512, 2048], P('tp'), may hold values from -0.25 to 0.25
Outputs:
- updated: bfloat16 [2048, 2048], P('sp', 'tp')
The draws below stay inside these ranges and needn't reach their ends.
Inputs may be any that keep to these rules, and one draw needn't show every extreme that they name: `routes`: each row names 4 different experts. In each aligned block of 256 rows (the rows of one index of sp) no expert is named by more than 64 rows, a bound that some block reaches.
All inputs are finite; a program needn't handle non-finite values.
Results may differ from the reference program's by a relative error of at most 0.0085.
Values may be sent and summed in bfloat16 or wider, within the bound.
A program may use at most 128 MiB of HBM per device.

```python
import math
import jax
import jax.numpy as jnp
import numpy as np
from jax import lax

D = 2048
HEADS = 8
DH = 96
FF = 512
TOP_K = 4
TOK_DEV = 256
TOKENS = 2048
EXPERTS = 32
CAP = 64
N_SP = 8
N_TP = 4


def draw_log_input_gate(key, part):
    base = jnp.clip(jax.random.normal(jax.random.fold_in(key, 11), (HEADS, TOKENS), jnp.float32), -4.0, 4.0)
    return base


def draw_forget_preactivation(key, part):
    noise = jnp.clip(jax.random.normal(jax.random.fold_in(key, 21), (HEADS, TOKENS), jnp.float32), -4.0, 4.0)
    blocks = TOKENS // TOK_DEV
    offsets = jax.random.uniform(jax.random.fold_in(key, 22), (HEADS, blocks), jnp.float32, -0.7, 0.7)
    which = jnp.arange(TOKENS, dtype=jnp.int32) // TOK_DEV
    return noise + jnp.take(offsets, which, axis=1)


def draw_head_forget_bias(key, part):
    order = jax.random.permutation(jax.random.fold_in(key, 31), HEADS)
    fast = order < HEADS // 2
    jitter = jax.random.uniform(jax.random.fold_in(key, 32), (HEADS,), jnp.float32, -0.5, 0.5)
    return jnp.where(fast, jnp.log(40.0), jnp.log(4.0 * TOKENS)) + jitter


def draw_forget_extra_boost(key, part):
    spots = jax.random.randint(jax.random.fold_in(key, 41), (HEADS, 2), 0, TOKENS)
    losses = jnp.log(jax.random.uniform(jax.random.fold_in(key, 42), (HEADS, 2), jnp.float32, 0.5, 0.8))
    places = jnp.arange(TOKENS, dtype=jnp.int32)[None, None, :]
    return jnp.sum(jnp.where(places == spots[:, :, None], losses[:, :, None], 0.0), axis=1)


def shard_levels(stream_key, dims, pieces, smallest, top_value):
    factor_of, own = 1.0, jax.random.fold_in(stream_key, 6)
    for dim, blocks in pieces:
        draws = jnp.exp(jax.random.uniform(jax.random.fold_in(own, dim), (blocks,), jnp.float32, smallest / len(pieces), top_value / len(pieces)))
        factor_of = factor_of * jnp.repeat(draws, dims[dim] // blocks).reshape([-1 if axis == dim else 1 for axis in range(len(dims))])
    return factor_of


def deal_out(own_key, own, number, rows, number_of, top, most, skew):
    order = jax.random.permutation(own_key, number_of)
    crowded, ordinary = shares(number_of, rows * top, most, skew, True), shares(number_of, rows * top, most, skew, False)
    places = jnp.arange(number_of)

    def named(sizes, offset_by):
        used = int((sizes > 0).sum())
        fixed = max(1, used // 4)
        passed = fixed + (places - fixed + offset_by * (used - fixed)) % max(1, number_of - fixed)
        return jnp.zeros((number_of,), jnp.int32).at[order[jnp.where(places < fixed, places, passed)]].set(jnp.asarray(sizes, jnp.int32))

    sizes = jnp.where(number % 4 == 0, named(crowded, number // 4), named(ordinary, number - number // 4 - 1))
    mixed = jax.random.permutation(jax.random.fold_in(own, 3), number_of)
    giver, taker = mixed[0:number_of // 2 * 2:2], mixed[1:number_of // 2 * 2:2]
    margin = jnp.minimum(sizes[giver] - 1, most - sizes[taker]) // 2
    margin = jnp.where((giver == order[0]) | (taker == order[0]) | (sizes[taker] == 0), 0, jnp.maximum(margin, 0))
    passed = jax.random.randint(jax.random.fold_in(own, 4), (number_of // 2,), 0, 1 << 20) % (margin + 1)
    sizes = sizes.at[giver].add(-passed).at[taker].add(passed)
    items = jnp.searchsorted(jnp.cumsum(sizes), jnp.arange(rows * top), side="right").astype(jnp.int32)
    listing = items.reshape(top, rows).T
    listing = listing[jax.random.permutation(jax.random.fold_in(own, 1), rows)]
    offset_by = jax.random.randint(jax.random.fold_in(own, 2), (rows, 1), 0, top)
    return jnp.take_along_axis(listing, (jnp.arange(top)[None, :] + offset_by) % top, axis=1)


def shares(amount, total, bound, lean, full):
    portions = [(1 << 20) // math.isqrt(grade ** lean) + 1 for grade in range(1, amount + 1)]
    largest = bound if full else min(bound, max(-(-total // amount), total * portions[0] // sum(portions)))
    least = 1 if total - largest >= amount - 1 else 0
    given, rest = [largest] + [least] * (amount - 1), total - largest - least * (amount - 1)
    while rest > 0:
        free = [i for i in range(1, amount) if given[i] < largest] or [i for i in range(1, amount) if given[i] < bound]
        mass, remaining = sum([portions[i] for i in free]), rest
        for i in free:
            addition = min(bound - given[i], max(1, remaining * portions[i] // mass), rest)
            given[i] = given[i] + addition
            rest = rest - addition
    return np.array(given)


def bell_draw(key, shape, spread, bound, pieces=(), held_as=jnp.bfloat16):
    loudness = shard_levels(key, shape, pieces, -0.22, 0.18) if pieces else 1.0
    drawn = jax.random.normal(key, shape, jnp.float32) * spread * loudness
    return jnp.minimum(jnp.maximum(drawn, -bound), bound).astype(held_as)


def setup_inputs(seed: int = 0) -> dict:
    streams_of = jax.random.split(jax.random.key(seed), 21)
    memory_queries = bell_draw(streams_of[0], (TOKENS, HEADS * DH), 1.0, 6.0, ((0, 8), (1, 4)))
    memory_keys = bell_draw(streams_of[1], (TOKENS, HEADS * DH), 1.0, 6.0, ((0, 8), (1, 4)))
    memory_values = bell_draw(streams_of[2], (TOKENS, HEADS * DH), 1.0, 6.0, ((0, 8), (1, 4)))
    output_gate_preactivation = bell_draw(streams_of[3], (TOKENS, HEADS * DH), 1.0, 6.0, ((0, 8), (1, 4)))
    log_input_gate = draw_log_input_gate(jax.random.fold_in(streams_of[20], 71), 0)
    forget_preactivation = draw_forget_preactivation(jax.random.fold_in(streams_of[20], 71), 0)
    head_forget_bias = draw_head_forget_bias(jax.random.fold_in(streams_of[20], 71), 0)
    forget_extra_boost = draw_forget_extra_boost(jax.random.fold_in(streams_of[20], 71), 0)
    head_norm_gain = jnp.clip(1.0 + 0.18 * jax.random.normal(streams_of[8], (HEADS * DH,), jnp.float32), 0.1, 1.9)
    memory_output_weight = bell_draw(streams_of[9], (HEADS * DH, D), (HEADS * DH) ** -0.5, 0.21875)
    residual = bell_draw(streams_of[10], (TOKENS, D), 1.0, 6.0, ((0, 8),))
    expert_norm_gain = jnp.clip(1.0 + 0.18 * jax.random.normal(streams_of[11], (D,), jnp.float32), 0.1, 1.9)
    routes_keys = jax.random.split(jax.random.fold_in(streams_of[12], 1), TOKENS // TOK_DEV)
    routes_turns = jax.random.permutation(jax.random.fold_in(streams_of[12], 3), TOKENS // TOK_DEV)
    routes = jax.vmap(lambda own, number: deal_out(jax.random.fold_in(streams_of[12], 2), own, number, TOK_DEV, EXPERTS, TOP_K, CAP, 1))(routes_keys, routes_turns).reshape((TOKENS, TOP_K))
    router_weight_matrix = jnp.clip(jnp.exp(math.log(1.0) - 2.3025851 * jax.random.uniform(streams_of[13], (TOKENS, TOP_K), jnp.float32) ** shard_levels(streams_of[13], (TOKENS, TOP_K), ((0, 8),), -0.2, 0.2)), 0.1, 1.0)
    routed_gate_weight = bell_draw(streams_of[14], (EXPERTS, D, FF), D ** -0.5, 0.125, ((0, 8), (2, 4)))
    routed_up_weight = bell_draw(streams_of[15], (EXPERTS, D, FF), D ** -0.5, 0.125, ((0, 8), (2, 4)))
    routed_down_weight = bell_draw(streams_of[16], (EXPERTS, FF, D), FF ** -0.5, 0.25, ((0, 8), (1, 4)))
    shared_gate_weight = bell_draw(streams_of[17], (D, FF), D ** -0.5, 0.125, ((1, 4),))
    shared_up_weight = bell_draw(streams_of[18], (D, FF), D ** -0.5, 0.125, ((1, 4),))
    shared_down_weight = bell_draw(streams_of[19], (FF, D), FF ** -0.5, 0.25, ((0, 4),))
    return dict(memory_queries=memory_queries, memory_keys=memory_keys, memory_values=memory_values, output_gate_preactivation=output_gate_preactivation, log_input_gate=log_input_gate, forget_preactivation=forget_preactivation, head_forget_bias=head_forget_bias, forget_extra_boost=forget_extra_boost, head_norm_gain=head_norm_gain, memory_output_weight=memory_output_weight, residual=residual, expert_norm_gain=expert_norm_gain, routes=routes, router_weight_matrix=router_weight_matrix, routed_gate_weight=routed_gate_weight, routed_up_weight=routed_up_weight, routed_down_weight=routed_down_weight, shared_gate_weight=shared_gate_weight, shared_up_weight=shared_up_weight, shared_down_weight=shared_down_weight)


NEG_LARGE = -1e+30
EPSILON = 1e-06

def matrix_memory_cell(memory_queries, memory_keys, memory_values, output_gate_preactivation, log_input_gate, forget_preactivation, head_forget_bias, forget_extra_boost, head_norm_gain):
    blocks = TOKENS // TOK_DEV
    scale = DH ** (-0.5)
    queries = memory_queries.reshape(blocks, TOK_DEV, HEADS, DH)
    keyset = memory_keys.reshape(blocks, TOK_DEV, HEADS, DH)
    valueset = memory_values.reshape(blocks, TOK_DEV, HEADS, DH)
    forget_log_gate = jax.nn.log_sigmoid(forget_preactivation + head_forget_bias[:, None]) + forget_extra_boost
    forget_log_gate = forget_log_gate.reshape(HEADS, blocks, TOK_DEV).transpose(1, 0, 2)
    log_input = log_input_gate.reshape(HEADS, blocks, TOK_DEV).transpose(1, 0, 2)
    causal = jnp.tril(jnp.ones((TOK_DEV, TOK_DEV), bool))

    def advance(carry, inputs):
        memory, stabil = carry
        q_block, k_block, v_block, i_block, f_block = inputs
        cumul = jnp.cumsum(f_block, axis=1)
        d_log = jnp.where(causal[None], cumul[:, :, None] - cumul[:, None, :] + i_block[:, None, :], NEG_LARGE)
        g_log = cumul + stabil[:, None]
        top = jnp.maximum(g_log, lax.optimization_barrier(jnp.max(d_log, axis=2)))
        q_float = q_block.astype(jnp.float32)
        k_float = k_block.astype(jnp.float32)
        v_float = v_block.astype(jnp.float32)
        scores = jnp.einsum('thd,shd->hts', q_float, k_float, precision=lax.Precision.HIGHEST) * scale
        weights = scores * jnp.exp(d_log - top[:, :, None])
        rounded = lax.optimization_barrier(weights.astype(jnp.bfloat16)).astype(jnp.float32)
        inter = jnp.exp(g_log - top)
        q_scaled = q_float * scale
        numer = jnp.einsum('hts,shd->thd', rounded, v_float, precision=lax.Precision.HIGHEST)
        hidden = numer + inter.T[:, :, None] * jnp.einsum('thd,hde->the', q_scaled, memory, precision=lax.Precision.HIGHEST)
        ending = cumul[:, -1]
        w_log = ending[:, None] - cumul + i_block
        new_top = jnp.maximum(ending + stabil, lax.optimization_barrier(jnp.max(w_log, axis=1)))
        w_end = jnp.exp(w_log - new_top[:, None])
        decay = jnp.exp(ending + stabil - new_top)
        memory = decay[:, None, None] * memory + jnp.einsum('hs,shd,she->hde', w_end, k_float, v_float, precision=lax.Precision.HIGHEST)
        return ((memory, new_top), hidden)
    start = (jnp.zeros((HEADS, DH, DH), jnp.float32), jnp.full((HEADS,), NEG_LARGE, jnp.float32))
    _, hiddens = lax.scan(advance, start, (queries, keyset, valueset, log_input, forget_log_gate))
    hiddens = hiddens.reshape(TOKENS, HEADS, DH)
    hiddens = hiddens * lax.rsqrt(lax.optimization_barrier(jnp.mean(hiddens * hiddens, axis=2, keepdims=True)) + EPSILON)
    gated = hiddens.reshape(TOKENS, HEADS * DH) * head_norm_gain * jax.nn.sigmoid(output_gate_preactivation.astype(jnp.float32))
    return gated.astype(jnp.bfloat16)

def reference(memory_queries, memory_keys, memory_values, output_gate_preactivation, log_input_gate, forget_preactivation, head_forget_bias, forget_extra_boost, head_norm_gain, memory_output_weight, residual, expert_norm_gain, routes, router_weight_matrix, routed_gate_weight, routed_up_weight, routed_down_weight, shared_gate_weight, shared_up_weight, shared_down_weight):
    token_mixing = matrix_memory_cell(memory_queries, memory_keys, memory_values, output_gate_preactivation, log_input_gate, forget_preactivation, head_forget_bias, forget_extra_boost, head_norm_gain)
    stream = residual.astype(jnp.float32) + jnp.dot(token_mixing, memory_output_weight, preferred_element_type=jnp.float32)
    normed = (stream * lax.rsqrt(lax.optimization_barrier(jnp.mean(stream * stream, axis=1, keepdims=True)) + EPSILON) * expert_norm_gain).astype(jnp.bfloat16)
    group = FF // N_TP
    most_rows = N_SP * CAP
    flat_routes = routes.reshape(-1)
    flat_owner = jnp.arange(TOKENS * TOP_K, dtype=jnp.int32) // TOP_K
    flat_weight = router_weight_matrix.reshape(-1)
    order = jnp.argsort(flat_routes, stable=True)
    sorted_owner = jnp.concatenate([flat_owner[order], jnp.zeros((most_rows,), jnp.int32)])
    sorted_weight = jnp.concatenate([flat_weight[order], jnp.zeros((most_rows,), jnp.float32)])
    counts = jnp.bincount(flat_routes, length=EXPERTS).astype(jnp.int32)
    starts = (jnp.cumsum(counts) - counts).astype(jnp.int32)
    lanes = jnp.arange(most_rows, dtype=jnp.int32)

    def one_expert(total, expert):
        valid = lanes < counts[expert]
        owners = lax.dynamic_slice(sorted_owner, (starts[expert],), (most_rows,))
        weights = lax.dynamic_slice(sorted_weight, (starts[expert],), (most_rows,))
        owners = jnp.where(valid, owners, 0).astype(jnp.int32)
        weights = jnp.where(valid, weights, 0.0)
        picked = normed[owners]
        gate_vals = jnp.dot(picked, routed_gate_weight[expert], preferred_element_type=jnp.float32)
        up_vals = jnp.dot(picked, routed_up_weight[expert], preferred_element_type=jnp.float32)
        hidden = (jax.nn.silu(gate_vals) * up_vals).astype(jnp.bfloat16)
        hidden_groups = hidden.reshape(most_rows, N_TP, group).astype(jnp.float32)
        down_groups = routed_down_weight[expert].reshape(N_TP, group, D).astype(jnp.float32)
        partials = jnp.einsum('rjf,jfd->rjd', hidden_groups, down_groups, precision=lax.Precision.HIGHEST)
        partials = partials.astype(jnp.bfloat16).astype(jnp.float32)
        output = lax.optimization_barrier(jnp.sum(partials, axis=1)).astype(jnp.bfloat16).astype(jnp.float32)
        return (total.at[owners].add(weights[:, None] * output), None)
    routed, _ = lax.scan(one_expert, jnp.zeros((TOKENS, D), jnp.float32), jnp.arange(EXPERTS, dtype=jnp.int32))
    shared_hidden = (jax.nn.silu(jnp.dot(normed, shared_gate_weight, preferred_element_type=jnp.float32)) * jnp.dot(normed, shared_up_weight, preferred_element_type=jnp.float32)).astype(jnp.bfloat16)
    shared = jnp.zeros((TOKENS, D), jnp.float32)
    for index in range(N_TP):
        piece = jnp.dot(shared_hidden[:, index * group:(index + 1) * group], shared_down_weight[index * group:(index + 1) * group], preferred_element_type=jnp.float32)
        shared = shared + piece.astype(jnp.bfloat16).astype(jnp.float32)
    return (stream + routed + shared).astype(jnp.bfloat16)
```

```python
import jax
import jax.numpy as jnp
from jax import lax
from jax.experimental import pallas as pl
from jax.experimental.pallas import tpu as pltpu
from jax.sharding import PartitionSpec as P

NEG_LARGE = -1e30
EPSILON = 1e-06


def spreads(experts_total, top_count):
    return experts_total <= 16 * top_count


def entering(local_memory, local_top, ending, routes, router_weight_matrix):
    count, here = (lax.axis_size("sp"), lax.axis_index("sp"))
    heads_here, head_size, _ = local_memory.shape
    top_count = routes.shape[1]
    lanes = -(-head_size // 128) * 128
    rows = heads_here * head_size
    memory_rows = jnp.pad(local_memory.reshape(rows, head_size), ((0, 0), (0, lanes - head_size)))
    logs = jnp.pad(jnp.stack([local_top, ending]), ((0, 6), (0, lanes - heads_here)))
    routing = jnp.concatenate([routes.astype(jnp.float32).T, router_weight_matrix.T], axis=0)
    packed = jnp.concatenate([memory_rows, logs, routing.reshape(-1, lanes)], axis=0)
    everything = lax.all_gather(packed, "sp")
    memories = everything[:, :rows, :head_size].reshape(count, heads_here, head_size, head_size)
    tops = everything[:, rows, :heads_here]
    totals = everything[:, rows + 1, :heads_here]
    routing_all = everything[:, rows + 8 :].reshape(count, 2 * top_count, -1)
    block = jnp.arange(count, dtype=jnp.int32)
    between = (block[None, :] > block[:, None]) & (block[None, :] < here)
    later = jnp.sum(jnp.where(between[:, :, None], totals[None], 0.0), axis=1)
    reached = (block < here)[:, None]
    logs_all = jnp.where(reached, tops + later, NEG_LARGE)
    stabil = jnp.max(logs_all, axis=0)
    share = jnp.where(reached, jnp.exp(logs_all - stabil[None]), 0.0)
    memory = jnp.sum(share[:, :, None, None] * memories, axis=0)
    return memory, stabil, routing_all[:, :top_count], routing_all[:, top_count:]


def experts_kernel(
    here_ref, x_ref, weight_ref, gate_ref, up_ref, down_ref,
    shared_gate_ref, shared_up_ref, shared_down_ref, out_ref, both_ref, hidden_ref,
):
    block = pl.program_id(0)
    experts, _, width = gate_ref.shape
    pieces, out_width = out_ref.shape[1], out_ref.shape[3]

    @pl.when(block == 0)
    def _():
        for e in range(experts):
            both_ref[e, :, :width] = gate_ref[e]
            both_ref[e, :, width:] = up_ref[e]
        both_ref[experts, :, :width] = shared_gate_ref[...]
        both_ref[experts, :, width:] = shared_up_ref[...]

    def hidden_of(e):
        both = jnp.dot(x_ref[...], both_ref[e], preferred_element_type=jnp.float32)
        return jax.nn.silu(both[:, :width]) * both[:, width:]

    for e in range(experts):
        hidden_ref[:, e * width : (e + 1) * width] = (
            hidden_of(e) * weight_ref[:, e : e + 1]
        ).astype(jnp.bfloat16)

    def piece_of(j):
        columns = slice(j * out_width, (j + 1) * out_width)
        total = jnp.dot(
            hidden_ref[:, :width], down_ref[0, :, columns], preferred_element_type=jnp.float32
        )
        for e in range(1, experts):
            total += jnp.dot(
                hidden_ref[:, e * width : (e + 1) * width],
                down_ref[e, :, columns],
                preferred_element_type=jnp.float32,
            )
        return total

    @pl.when(block == here_ref[0])
    def _():
        shared_hidden = hidden_of(experts).astype(jnp.bfloat16)
        for j in range(pieces):
            columns = slice(j * out_width, (j + 1) * out_width)
            out_ref[0, j] = (
                piece_of(j)
                + jnp.dot(
                    shared_hidden, shared_down_ref[:, columns], preferred_element_type=jnp.float32
                )
            ).astype(jnp.bfloat16)

    @pl.when(block != here_ref[0])
    def _():
        for j in range(pieces):
            out_ref[0, j] = piece_of(j).astype(jnp.bfloat16)


def spread_experts(
    stream,
    normed,
    all_routes,
    all_weights,
    routed_gate_weight,
    routed_up_weight,
    routed_down_weight,
    shared_gate_weight,
    shared_up_weight,
    shared_down_weight,
):
    tokens_here, model_width = normed.shape
    sp_count, tp_count = (lax.axis_size("sp"), lax.axis_size("tp"))
    sp_index, tp_index = (lax.axis_index("sp"), lax.axis_index("tp"))
    local_experts, _, width = routed_gate_weight.shape
    part = tokens_here // tp_count
    width_share = model_width // tp_count
    mine = lax.dynamic_slice_in_dim(normed, tp_index * part, part, 0)
    rows = lax.all_gather(mine, ("sp", "tp"), axis=0, tiled=True)
    first = (sp_index * local_experts).astype(jnp.float32)
    named = first + jnp.arange(local_experts, dtype=jnp.float32)
    weight = jnp.sum(
        jnp.where(all_routes[:, :, None, :] == named[None, None, :, None], all_weights[:, :, None, :], 0.0),
        axis=1,
    )
    weight = weight.transpose(0, 2, 1).reshape(sp_count * tokens_here, local_experts)
    whole = lambda *shape: pl.BlockSpec(shape, lambda b, here: (0,) * len(shape))
    partial = pl.pallas_call(
        experts_kernel,
        out_shape=jax.ShapeDtypeStruct((sp_count, tp_count, tokens_here, width_share), jnp.bfloat16),
        grid_spec=pltpu.PrefetchScalarGridSpec(
            num_scalar_prefetch=1,
            grid=(sp_count,),
            in_specs=[
                pl.BlockSpec((tokens_here, model_width), lambda b, here: (b, 0)),
                pl.BlockSpec((tokens_here, local_experts), lambda b, here: (b, 0)),
                whole(*routed_gate_weight.shape),
                whole(*routed_up_weight.shape),
                whole(*routed_down_weight.shape),
                whole(*shared_gate_weight.shape),
                whole(*shared_up_weight.shape),
                whole(*shared_down_weight.shape),
            ],
            out_specs=pl.BlockSpec(
                (1, tp_count, tokens_here, width_share), lambda b, here: (b, 0, 0, 0)
            ),
            scratch_shapes=[
                pltpu.VMEM((local_experts + 1, model_width, 2 * width), jnp.bfloat16),
                pltpu.VMEM((tokens_here, local_experts * width), jnp.bfloat16),
            ],
        ),
        compiler_params=pltpu.CompilerParams(dimension_semantics=("arbitrary",)),
    )(
        sp_index.astype(jnp.int32).reshape(1),
        rows,
        weight,
        routed_gate_weight,
        routed_up_weight,
        routed_down_weight,
        shared_gate_weight,
        shared_up_weight,
        shared_down_weight,
    )
    combined = lax.psum_scatter(
        partial.reshape(sp_count * tp_count, tokens_here, width_share),
        ("sp", "tp"),
        scatter_dimension=0,
        tiled=True,
    ).reshape(tokens_here, width_share)
    stream_share = lax.dynamic_slice_in_dim(stream, tp_index * width_share, width_share, 1)
    return (stream_share + combined.astype(jnp.float32)).astype(jnp.bfloat16)


def exchange_experts(
    stream,
    normed,
    routes,
    router_weight_matrix,
    routed_gate_weight,
    routed_up_weight,
    routed_down_weight,
    shared_gate_weight,
    shared_up_weight,
    shared_down_weight,
):
    tokens_here, model_width = normed.shape
    sp_count = lax.axis_size("sp")
    tp_count = lax.axis_size("tp")
    tp_index = lax.axis_index("tp")
    local_experts = routed_gate_weight.shape[0]
    experts_total = local_experts * sp_count
    top_count = routes.shape[1]
    capacity = 2 * tokens_here * top_count // experts_total
    width_share = model_width // tp_count
    flat_routes = routes.reshape(-1)
    onehot = (flat_routes[:, None] == jnp.arange(experts_total, dtype=jnp.int32)[None, :]).astype(
        jnp.int32
    )
    earlier_count = jnp.cumsum(onehot, axis=0) - onehot
    slot_index = jnp.sum(earlier_count * onehot, axis=1)
    position = flat_routes * capacity + slot_index
    owner = jnp.arange(flat_routes.shape[0], dtype=jnp.int32) // top_count
    slot_token = (
        jnp.full((experts_total * capacity,), tokens_here, jnp.int32).at[position].set(owner)
    )
    padded = jnp.concatenate([normed, jnp.zeros((1, model_width), jnp.bfloat16)], axis=0)
    shared_hidden = (
        jax.nn.silu(jnp.dot(normed, shared_gate_weight, preferred_element_type=jnp.float32))
        * jnp.dot(normed, shared_up_weight, preferred_element_type=jnp.float32)
    ).astype(jnp.bfloat16)
    shared_partial = jnp.dot(shared_hidden, shared_down_weight, preferred_element_type=jnp.float32)
    stream_share = lax.dynamic_slice_in_dim(stream, tp_index * width_share, width_share, 1)
    group_count = local_experts // tp_count
    whole_gate, whole_up = (
        lax.all_to_all(routed_gate_weight, "tp", split_axis=0, concat_axis=2, tiled=True),
        lax.all_to_all(routed_up_weight, "tp", split_axis=0, concat_axis=2, tiled=True),
    )
    whole_down = lax.all_to_all(routed_down_weight, "tp", split_axis=0, concat_axis=1, tiled=True)
    slot_table = slot_token.reshape(sp_count, local_experts, capacity)
    chosen = lax.dynamic_slice_in_dim(slot_table, tp_index * group_count, group_count, 1)
    outgoing = jnp.take(padded, chosen.reshape(-1), axis=0).reshape(
        sp_count, group_count, capacity, model_width
    )
    arrived = lax.all_to_all(outgoing, "sp", split_axis=0, concat_axis=0, tiled=True)
    gate_vals = jnp.einsum(
        "secd,edf->secf", arrived, whole_gate, preferred_element_type=jnp.float32
    )
    up_vals = jnp.einsum("secd,edf->secf", arrived, whole_up, preferred_element_type=jnp.float32)
    expert_hidden = (jax.nn.silu(gate_vals) * up_vals).astype(jnp.bfloat16)
    hidden_width = whole_down.shape[1]
    group_width = hidden_width // tp_count
    expert_sum = jnp.zeros(arrived.shape[:3] + (model_width,), jnp.float32)
    for index in range(tp_count):
        piece = jnp.einsum(
            "secf,efd->secd",
            expert_hidden[..., index * group_width : (index + 1) * group_width],
            whole_down[:, index * group_width : (index + 1) * group_width, :],
            preferred_element_type=jnp.float32,
        )
        expert_sum = expert_sum + piece.astype(jnp.bfloat16).astype(jnp.float32)
    expert_rows = expert_sum.astype(jnp.bfloat16)
    back = lax.all_to_all(expert_rows, "sp", split_axis=0, concat_axis=0, tiled=True)
    back_flat = back.reshape(sp_count * group_count * capacity, model_width)
    owner_sp = flat_routes // local_experts
    local_slot = flat_routes % local_experts - tp_index * group_count
    belongs = (local_slot >= 0) & (local_slot < group_count)
    local_position = jnp.where(
        belongs, (owner_sp * group_count + local_slot) * capacity + slot_index, 0
    )
    picked = jnp.take(back_flat, local_position, axis=0).reshape(
        tokens_here, top_count, model_width
    )
    kept_weight = jnp.where(belongs.reshape(tokens_here, top_count), router_weight_matrix, 0.0)
    routed_partial = jnp.sum(kept_weight[:, :, None] * picked.astype(jnp.float32), axis=1)
    shared_rounded = shared_partial.astype(jnp.bfloat16).astype(jnp.float32)
    combined = lax.psum_scatter(
        (routed_partial + shared_rounded).astype(jnp.bfloat16),
        "tp",
        scatter_dimension=1,
        tiled=True,
    ).astype(jnp.float32)
    return (stream_share + combined).astype(jnp.bfloat16)


def body(
    memory_queries,
    memory_keys,
    memory_values,
    output_gate_preactivation,
    log_input_gate,
    forget_preactivation,
    head_forget_bias,
    forget_extra_boost,
    head_norm_gain,
    memory_output_weight,
    residual,
    expert_norm_gain,
    routes,
    router_weight_matrix,
    routed_gate_weight,
    routed_up_weight,
    routed_down_weight,
    shared_gate_weight,
    shared_up_weight,
    shared_down_weight,
):
    tokens_here = memory_queries.shape[0]
    heads_here = log_input_gate.shape[0]
    head_size = memory_queries.shape[1] // heads_here
    scale = head_size ** (-0.5)
    queries = memory_queries.reshape(tokens_here, heads_here, head_size)
    keyset = memory_keys.reshape(tokens_here, heads_here, head_size)
    valueset = memory_values.reshape(tokens_here, heads_here, head_size)
    forget_log_gate = (
        jax.nn.log_sigmoid(forget_preactivation + head_forget_bias[:, None]) + forget_extra_boost
    )
    cumul = jnp.cumsum(forget_log_gate, axis=1)
    causal = jnp.tril(jnp.ones((tokens_here, tokens_here), bool))
    d_log = jnp.where(
        causal[None], cumul[:, :, None] - cumul[:, None, :] + log_input_gate[:, None, :], NEG_LARGE
    )
    ending = cumul[:, -1]
    w_log = ending[:, None] - cumul + log_input_gate
    local_top = jnp.max(w_log, axis=1)
    w_end = jnp.exp(w_log - local_top[:, None])
    keys_float = keyset.astype(jnp.float32)
    values_float = valueset.astype(jnp.float32)
    local_memory = jnp.einsum(
        "hs,shd,she->hde", w_end, keys_float, values_float, precision=lax.Precision.HIGHEST
    )
    memory, stabil, all_routes, all_weights = entering(
        local_memory, local_top, ending, routes, router_weight_matrix
    )
    g_log = cumul + stabil[:, None]
    top = jnp.maximum(g_log, jnp.max(d_log, axis=2))
    scores = jnp.einsum("thd,shd->hts", queries, keyset, preferred_element_type=jnp.float32) * scale
    weights = scores * jnp.exp(d_log - top[:, :, None])
    inter = jnp.exp(g_log - top)
    q_scaled = queries.astype(jnp.float32) * scale
    numer = jnp.einsum(
        "hts,shd->thd", weights.astype(jnp.bfloat16), valueset, preferred_element_type=jnp.float32
    )
    hidden = numer + inter.T[:, :, None] * jnp.einsum(
        "thd,hde->the", q_scaled, memory, precision=lax.Precision.HIGHEST
    )
    hidden = hidden * lax.rsqrt(jnp.mean(hidden * hidden, axis=2, keepdims=True) + EPSILON)
    token_mixing = (
        hidden.reshape(tokens_here, heads_here * head_size)
        * head_norm_gain
        * jax.nn.sigmoid(output_gate_preactivation.astype(jnp.float32))
    ).astype(jnp.bfloat16)
    mixed = jnp.dot(
        lax.all_gather(token_mixing, "tp", axis=1, tiled=True),
        memory_output_weight,
        preferred_element_type=jnp.float32,
    )
    stream = residual.astype(jnp.float32) + mixed
    normed = (
        stream
        * lax.rsqrt(jnp.mean(stream * stream, axis=1, keepdims=True) + EPSILON)
        * expert_norm_gain
    ).astype(jnp.bfloat16)
    weights_here = (
        routed_gate_weight,
        routed_up_weight,
        routed_down_weight,
        shared_gate_weight,
        shared_up_weight,
        shared_down_weight,
    )
    experts_total = routed_gate_weight.shape[0] * lax.axis_size("sp")
    if spreads(experts_total, routes.shape[1]):
        return spread_experts(stream, normed, all_routes, all_weights, *weights_here)
    return exchange_experts(stream, normed, routes, router_weight_matrix, *weights_here)


def solution(mesh):
    in_specs = (
        P("sp", "tp"),
        P("sp", "tp"),
        P("sp", "tp"),
        P("sp", "tp"),
        P("tp", "sp"),
        P("tp", "sp"),
        P("tp"),
        P("tp", "sp"),
        P("tp"),
        P(),
        P("sp", None),
        P(),
        P("sp", None),
        P("sp", None),
        P("sp", None, "tp"),
        P("sp", None, "tp"),
        P("sp", "tp", None),
        P(None, "tp"),
        P(None, "tp"),
        P("tp", None),
    )
    out_specs = P("sp", "tp")
    return jax.shard_map(body, mesh=mesh, in_specs=in_specs, out_specs=out_specs, check_vma=False)
```

```python
import jax
import jax.numpy as jnp
from jax import lax
from jax.experimental import pallas as pl
from jax.experimental.pallas import tpu as pltpu
from jax.sharding import PartitionSpec as P

NEG_LARGE = -1e30
EPSILON = 1e-06


def spreads(experts_total, top_count, tp_count):
    return experts_total <= 16 * top_count and tp_count == 4


def entering(local_memory, local_top, ending, routes, router_weight_matrix):
    count, here = (lax.axis_size("sp"), lax.axis_index("sp"))
    heads_here, head_size, _ = local_memory.shape
    top_count = routes.shape[1]
    lanes = -(-head_size // 128) * 128
    rows = heads_here * head_size
    memory_rows = jnp.pad(local_memory.reshape(rows, head_size), ((0, 0), (0, lanes - head_size)))
    logs = jnp.pad(jnp.stack([local_top, ending]), ((0, 6), (0, lanes - heads_here)))
    routing = jnp.concatenate([routes.astype(jnp.float32).T, router_weight_matrix.T], axis=0)
    packed = jnp.concatenate([memory_rows, logs, routing.reshape(-1, lanes)], axis=0)
    everything = lax.all_gather(packed, "sp")
    memories = everything[:, :rows, :head_size].reshape(count, heads_here, head_size, head_size)
    tops = everything[:, rows, :heads_here]
    totals = everything[:, rows + 1, :heads_here]
    routing_all = everything[:, rows + 8 :].reshape(count, 2 * top_count, -1)
    block = jnp.arange(count, dtype=jnp.int32)
    between = (block[None, :] > block[:, None]) & (block[None, :] < here)
    later = jnp.sum(jnp.where(between[:, :, None], totals[None], 0.0), axis=1)
    reached = (block < here)[:, None]
    logs_all = jnp.where(reached, tops + later, NEG_LARGE)
    stabil = jnp.max(logs_all, axis=0)
    share = jnp.where(reached, jnp.exp(logs_all - stabil[None]), 0.0)
    memory = jnp.sum(share[:, :, None, None] * memories, axis=0)
    return memory, stabil, routing_all[:, :top_count], routing_all[:, top_count:]


def experts_kernel(
    here_ref, x_ref, weight_ref, gate_ref, up_ref, down_ref,
    shared_gate_ref, shared_up_ref, shared_down_ref, out_ref, both_ref, hidden_ref,
):
    block = pl.program_id(0)
    experts, _, width = gate_ref.shape
    pieces, out_width = out_ref.shape[1], out_ref.shape[3]

    @pl.when(block == 0)
    def _():
        for e in range(experts):
            both_ref[e, :, :width] = gate_ref[e]
            both_ref[e, :, width:] = up_ref[e]
        both_ref[experts, :, :width] = shared_gate_ref[...]
        both_ref[experts, :, width:] = shared_up_ref[...]

    def hidden_of(e):
        both = jnp.dot(x_ref[...], both_ref[e], preferred_element_type=jnp.float32)
        return jax.nn.silu(both[:, :width]) * both[:, width:]

    for e in range(experts):
        hidden_ref[:, e * width : (e + 1) * width] = (
            hidden_of(e) * weight_ref[:, e : e + 1]
        ).astype(jnp.bfloat16)

    def piece_of(j):
        columns = slice(j * out_width, (j + 1) * out_width)
        total = jnp.dot(
            hidden_ref[:, :width], down_ref[0, :, columns], preferred_element_type=jnp.float32
        )
        for e in range(1, experts):
            total += jnp.dot(
                hidden_ref[:, e * width : (e + 1) * width],
                down_ref[e, :, columns],
                preferred_element_type=jnp.float32,
            )
        return total

    @pl.when(block == here_ref[0])
    def _():
        shared_hidden = hidden_of(experts).astype(jnp.bfloat16)
        for j in range(pieces):
            columns = slice(j * out_width, (j + 1) * out_width)
            out_ref[0, j] = (
                piece_of(j)
                + jnp.dot(
                    shared_hidden, shared_down_ref[:, columns], preferred_element_type=jnp.float32
                )
            ).astype(jnp.bfloat16)

    @pl.when(block != here_ref[0])
    def _():
        for j in range(pieces):
            out_ref[0, j] = piece_of(j).astype(jnp.bfloat16)


def ring_order(count):
    return list(range(0, count, 2)) + list(range(count - 1, 0, -2))


def add_rounded(a, b):
    return (a.astype(jnp.float32) + b.astype(jnp.float32)).astype(jnp.bfloat16)


def reduce_scatter(partial):
    sp_count, tp_count, tokens, width = partial.shape
    sp_index, tp_index = (lax.axis_index("sp"), lax.axis_index("tp"))
    near, far = tp_index % 2, tp_index // 2
    pairs = partial.reshape(sp_count, tp_count // 2, 2, tokens, width)
    swap_near = [(i, i ^ 1) for i in range(tp_count)]
    given = lax.dynamic_index_in_dim(pairs, 1 - near, 2, keepdims=False)
    kept = lax.dynamic_index_in_dim(pairs, near, 2, keepdims=False)
    kept = add_rounded(kept, lax.ppermute(given, "tp", swap_near))

    order = ring_order(sp_count)
    place_of = [order.index(i) for i in range(sp_count)]
    place = jnp.asarray(place_of, jnp.int32)[sp_index]
    order_array = jnp.asarray(order, jnp.int32)
    half = tokens // 2
    sums = []
    for turn, rows in ((1, slice(0, half)), (-1, slice(half, tokens))):
        links = [(order[p], order[(p + turn) % sp_count]) for p in range(sp_count)]

        def block(k):
            owner = order_array[(place - turn * k) % sp_count]
            return lax.dynamic_index_in_dim(kept[:, :, rows], owner, 0, keepdims=False)

        moving = block(1)
        for k in range(2, sp_count + 1):
            moving = add_rounded(lax.ppermute(moving, "sp", links), block(k))
        sums.append(moving)
    mine = jnp.concatenate(sums, axis=1)
    swap_far = [(i, (i + 2) % tp_count) for i in range(tp_count)]
    given = lax.dynamic_index_in_dim(mine, 1 - far, 0, keepdims=False)
    kept = lax.dynamic_index_in_dim(mine, far, 0, keepdims=False)
    return kept.astype(jnp.float32) + lax.ppermute(given, "tp", swap_far).astype(jnp.float32)


def spread_experts(
    stream,
    normed,
    all_routes,
    all_weights,
    routed_gate_weight,
    routed_up_weight,
    routed_down_weight,
    shared_gate_weight,
    shared_up_weight,
    shared_down_weight,
):
    tokens_here, model_width = normed.shape
    sp_count, tp_count = (lax.axis_size("sp"), lax.axis_size("tp"))
    sp_index, tp_index = (lax.axis_index("sp"), lax.axis_index("tp"))
    local_experts, _, width = routed_gate_weight.shape
    part = tokens_here // tp_count
    width_share = model_width // tp_count
    mine = lax.dynamic_slice_in_dim(normed, tp_index * part, part, 0)
    rows = lax.all_gather(mine, ("sp", "tp"), axis=0, tiled=True)
    first = (sp_index * local_experts).astype(jnp.float32)
    named = first + jnp.arange(local_experts, dtype=jnp.float32)
    weight = jnp.sum(
        jnp.where(all_routes[:, :, None, :] == named[None, None, :, None], all_weights[:, :, None, :], 0.0),
        axis=1,
    )
    weight = weight.transpose(0, 2, 1).reshape(sp_count * tokens_here, local_experts)
    whole = lambda *shape: pl.BlockSpec(shape, lambda b, here: (0,) * len(shape))
    partial = pl.pallas_call(
        experts_kernel,
        out_shape=jax.ShapeDtypeStruct((sp_count, tp_count, tokens_here, width_share), jnp.bfloat16),
        grid_spec=pltpu.PrefetchScalarGridSpec(
            num_scalar_prefetch=1,
            grid=(sp_count,),
            in_specs=[
                pl.BlockSpec((tokens_here, model_width), lambda b, here: (b, 0)),
                pl.BlockSpec((tokens_here, local_experts), lambda b, here: (b, 0)),
                whole(*routed_gate_weight.shape),
                whole(*routed_up_weight.shape),
                whole(*routed_down_weight.shape),
                whole(*shared_gate_weight.shape),
                whole(*shared_up_weight.shape),
                whole(*shared_down_weight.shape),
            ],
            out_specs=pl.BlockSpec(
                (1, tp_count, tokens_here, width_share), lambda b, here: (b, 0, 0, 0)
            ),
            scratch_shapes=[
                pltpu.VMEM((local_experts + 1, model_width, 2 * width), jnp.bfloat16),
                pltpu.VMEM((tokens_here, local_experts * width), jnp.bfloat16),
            ],
        ),
        compiler_params=pltpu.CompilerParams(dimension_semantics=("arbitrary",)),
    )(
        sp_index.astype(jnp.int32).reshape(1),
        rows,
        weight,
        routed_gate_weight,
        routed_up_weight,
        routed_down_weight,
        shared_gate_weight,
        shared_up_weight,
        shared_down_weight,
    )
    combined = reduce_scatter(partial)
    stream_share = lax.dynamic_slice_in_dim(stream, tp_index * width_share, width_share, 1)
    return (stream_share + combined.astype(jnp.float32)).astype(jnp.bfloat16)


def exchange_experts(
    stream,
    normed,
    routes,
    router_weight_matrix,
    routed_gate_weight,
    routed_up_weight,
    routed_down_weight,
    shared_gate_weight,
    shared_up_weight,
    shared_down_weight,
):
    tokens_here, model_width = normed.shape
    sp_count = lax.axis_size("sp")
    tp_count = lax.axis_size("tp")
    tp_index = lax.axis_index("tp")
    local_experts = routed_gate_weight.shape[0]
    experts_total = local_experts * sp_count
    top_count = routes.shape[1]
    capacity = 2 * tokens_here * top_count // experts_total
    width_share = model_width // tp_count
    flat_routes = routes.reshape(-1)
    onehot = (flat_routes[:, None] == jnp.arange(experts_total, dtype=jnp.int32)[None, :]).astype(
        jnp.int32
    )
    earlier_count = jnp.cumsum(onehot, axis=0) - onehot
    slot_index = jnp.sum(earlier_count * onehot, axis=1)
    position = flat_routes * capacity + slot_index
    owner = jnp.arange(flat_routes.shape[0], dtype=jnp.int32) // top_count
    slot_token = (
        jnp.full((experts_total * capacity,), tokens_here, jnp.int32).at[position].set(owner)
    )
    padded = jnp.concatenate([normed, jnp.zeros((1, model_width), jnp.bfloat16)], axis=0)
    shared_hidden = (
        jax.nn.silu(jnp.dot(normed, shared_gate_weight, preferred_element_type=jnp.float32))
        * jnp.dot(normed, shared_up_weight, preferred_element_type=jnp.float32)
    ).astype(jnp.bfloat16)
    shared_partial = jnp.dot(shared_hidden, shared_down_weight, preferred_element_type=jnp.float32)
    stream_share = lax.dynamic_slice_in_dim(stream, tp_index * width_share, width_share, 1)
    group_count = local_experts // tp_count
    whole_gate, whole_up = (
        lax.all_to_all(routed_gate_weight, "tp", split_axis=0, concat_axis=2, tiled=True),
        lax.all_to_all(routed_up_weight, "tp", split_axis=0, concat_axis=2, tiled=True),
    )
    whole_down = lax.all_to_all(routed_down_weight, "tp", split_axis=0, concat_axis=1, tiled=True)
    slot_table = slot_token.reshape(sp_count, local_experts, capacity)
    chosen = lax.dynamic_slice_in_dim(slot_table, tp_index * group_count, group_count, 1)
    outgoing = jnp.take(padded, chosen.reshape(-1), axis=0).reshape(
        sp_count, group_count, capacity, model_width
    )
    arrived = lax.all_to_all(outgoing, "sp", split_axis=0, concat_axis=0, tiled=True)
    gate_vals = jnp.einsum(
        "secd,edf->secf", arrived, whole_gate, preferred_element_type=jnp.float32
    )
    up_vals = jnp.einsum("secd,edf->secf", arrived, whole_up, preferred_element_type=jnp.float32)
    expert_hidden = (jax.nn.silu(gate_vals) * up_vals).astype(jnp.bfloat16)
    hidden_width = whole_down.shape[1]
    group_width = hidden_width // tp_count
    expert_sum = jnp.zeros(arrived.shape[:3] + (model_width,), jnp.float32)
    for index in range(tp_count):
        piece = jnp.einsum(
            "secf,efd->secd",
            expert_hidden[..., index * group_width : (index + 1) * group_width],
            whole_down[:, index * group_width : (index + 1) * group_width, :],
            preferred_element_type=jnp.float32,
        )
        expert_sum = expert_sum + piece.astype(jnp.bfloat16).astype(jnp.float32)
    expert_rows = expert_sum.astype(jnp.bfloat16)
    back = lax.all_to_all(expert_rows, "sp", split_axis=0, concat_axis=0, tiled=True)
    back_flat = back.reshape(sp_count * group_count * capacity, model_width)
    owner_sp = flat_routes // local_experts
    local_slot = flat_routes % local_experts - tp_index * group_count
    belongs = (local_slot >= 0) & (local_slot < group_count)
    local_position = jnp.where(
        belongs, (owner_sp * group_count + local_slot) * capacity + slot_index, 0
    )
    picked = jnp.take(back_flat, local_position, axis=0).reshape(
        tokens_here, top_count, model_width
    )
    kept_weight = jnp.where(belongs.reshape(tokens_here, top_count), router_weight_matrix, 0.0)
    routed_partial = jnp.sum(kept_weight[:, :, None] * picked.astype(jnp.float32), axis=1)
    shared_rounded = shared_partial.astype(jnp.bfloat16).astype(jnp.float32)
    combined = lax.psum_scatter(
        (routed_partial + shared_rounded).astype(jnp.bfloat16),
        "tp",
        scatter_dimension=1,
        tiled=True,
    ).astype(jnp.float32)
    return (stream_share + combined).astype(jnp.bfloat16)


def body(
    memory_queries,
    memory_keys,
    memory_values,
    output_gate_preactivation,
    log_input_gate,
    forget_preactivation,
    head_forget_bias,
    forget_extra_boost,
    head_norm_gain,
    memory_output_weight,
    residual,
    expert_norm_gain,
    routes,
    router_weight_matrix,
    routed_gate_weight,
    routed_up_weight,
    routed_down_weight,
    shared_gate_weight,
    shared_up_weight,
    shared_down_weight,
):
    tokens_here = memory_queries.shape[0]
    heads_here = log_input_gate.shape[0]
    head_size = memory_queries.shape[1] // heads_here
    scale = head_size ** (-0.5)
    queries = memory_queries.reshape(tokens_here, heads_here, head_size)
    keyset = memory_keys.reshape(tokens_here, heads_here, head_size)
    valueset = memory_values.reshape(tokens_here, heads_here, head_size)
    forget_log_gate = (
        jax.nn.log_sigmoid(forget_preactivation + head_forget_bias[:, None]) + forget_extra_boost
    )
    cumul = jnp.cumsum(forget_log_gate, axis=1)
    causal = jnp.tril(jnp.ones((tokens_here, tokens_here), bool))
    d_log = jnp.where(
        causal[None], cumul[:, :, None] - cumul[:, None, :] + log_input_gate[:, None, :], NEG_LARGE
    )
    ending = cumul[:, -1]
    w_log = ending[:, None] - cumul + log_input_gate
    local_top = jnp.max(w_log, axis=1)
    w_end = jnp.exp(w_log - local_top[:, None])
    keys_float = keyset.astype(jnp.float32)
    values_float = valueset.astype(jnp.float32)
    local_memory = jnp.einsum(
        "hs,shd,she->hde", w_end, keys_float, values_float, precision=lax.Precision.HIGHEST
    )
    memory, stabil, all_routes, all_weights = entering(
        local_memory, local_top, ending, routes, router_weight_matrix
    )
    g_log = cumul + stabil[:, None]
    top = jnp.maximum(g_log, jnp.max(d_log, axis=2))
    scores = jnp.einsum("thd,shd->hts", queries, keyset, preferred_element_type=jnp.float32) * scale
    weights = scores * jnp.exp(d_log - top[:, :, None])
    inter = jnp.exp(g_log - top)
    q_scaled = queries.astype(jnp.float32) * scale
    numer = jnp.einsum(
        "hts,shd->thd", weights.astype(jnp.bfloat16), valueset, preferred_element_type=jnp.float32
    )
    hidden = numer + inter.T[:, :, None] * jnp.einsum(
        "thd,hde->the", q_scaled, memory, precision=lax.Precision.HIGHEST
    )
    hidden = hidden * lax.rsqrt(jnp.mean(hidden * hidden, axis=2, keepdims=True) + EPSILON)
    token_mixing = (
        hidden.reshape(tokens_here, heads_here * head_size)
        * head_norm_gain
        * jax.nn.sigmoid(output_gate_preactivation.astype(jnp.float32))
    ).astype(jnp.bfloat16)
    mixed = jnp.dot(
        lax.all_gather(token_mixing, "tp", axis=1, tiled=True),
        memory_output_weight,
        preferred_element_type=jnp.float32,
    )
    stream = residual.astype(jnp.float32) + mixed
    normed = (
        stream
        * lax.rsqrt(jnp.mean(stream * stream, axis=1, keepdims=True) + EPSILON)
        * expert_norm_gain
    ).astype(jnp.bfloat16)
    weights_here = (
        routed_gate_weight,
        routed_up_weight,
        routed_down_weight,
        shared_gate_weight,
        shared_up_weight,
        shared_down_weight,
    )
    experts_total = routed_gate_weight.shape[0] * lax.axis_size("sp")
    if spreads(experts_total, routes.shape[1], lax.axis_size("tp")):
        return spread_experts(stream, normed, all_routes, all_weights, *weights_here)
    return exchange_experts(stream, normed, routes, router_weight_matrix, *weights_here)


def solution(mesh):
    in_specs = (
        P("sp", "tp"),
        P("sp", "tp"),
        P("sp", "tp"),
        P("sp", "tp"),
        P("tp", "sp"),
        P("tp", "sp"),
        P("tp"),
        P("tp", "sp"),
        P("tp"),
        P(),
        P("sp", None),
        P(),
        P("sp", None),
        P("sp", None),
        P("sp", None, "tp"),
        P("sp", None, "tp"),
        P("sp", "tp", None),
        P(None, "tp"),
        P(None, "tp"),
        P("tp", None),
    )
    out_specs = P("sp", "tp")
    return jax.shard_map(body, mesh=mesh, in_specs=in_specs, out_specs=out_specs, check_vma=False)
```
